32 devices in a mesh: sp: 8 (over z, x), dp: 4 (over y, core).
Axes of the slice: x: 2, y: 2, z: 4, core: 2. Of those that a mesh axis runs over, the one named last changes fastest.
Arguments:
- gate_in: bfloat16 [4, 4096, 1024], P('dp', 'sp'), may hold values from -6 to 6
- value_in: bfloat16 [4, 4096, 1024], P('dp', 'sp'), may hold values from -6 to 6
- segments: int32 [4, 4096], P('dp', 'sp'), may hold values from 0 to 1, never falling along the last dimension, each value on 1 to 3072 neighbouring positions
- value_gain: bfloat16 [1024], P('sp'), may hold values from 0.099609375 to 1.8984375
- mixing: bfloat16 [8, 1024, 1024], P('sp', 'dp'), may hold values from -0.1875 to 0.1875
- mixing_bias: bfloat16 [8, 1024], P('sp'), may hold values from 0.099609375 to 1.8984375
Outputs:
- gated: bfloat16 [4, 4096, 1024], P('dp', 'sp')
The draws below stay inside these ranges and needn't reach their ends.
Inputs may be any that keep to these rules, and one draw needn't show every extreme that they name: `segments`: within each sequence the numbers never fall, every number 0 to 1 occurs, a document spans at most 3072 positions and some document spans exactly that.
All inputs are finite; a program needn't handle non-finite values.
Results may differ from the reference program's by a relative error of at most 0.0054.
Values may be sent and summed in bfloat16 or wider, within the bound.
A program may use at most 128 MiB of HBM per device.

```python
import math
import jax
import jax.numpy as jnp
import numpy as np
from jax import lax

HEAD_DIM = 128
HEADS = 8
WIDTH = 1024
BLK = 1024
TOK_DEV = 512
SEQ = 4096
SEQS = 4
DOCS = 2


def steps_of(rng, dims, pieces, low, top_value):
    loudness, own = 1.0, jax.random.fold_in(rng, 6)
    for position, parts in pieces:
        heights = jnp.exp(jax.random.uniform(jax.random.fold_in(own, position), (parts,), jnp.float32, low / len(pieces), top_value / len(pieces)))
        loudness = loudness * jnp.repeat(heights, dims[position] // parts).reshape([-1 if axis == position else 1 for axis in range(len(dims))])
    return loudness


def split_up(count, total, reach, skew):
    portions = [(1 << 20) // math.isqrt(standing ** skew) + 1 for standing in range(2, count + 1)]
    spare, given = total - reach - (count - 1), [1] * (count - 1)
    while spare > 0:
        candidates = [i for i in range(count - 1) if given[i] < reach]
        whole, remaining = sum([portions[i] for i in candidates]), spare
        for i in candidates:
            extra = min(reach - given[i], max(1, remaining * portions[i] // whole), spare)
            given[i] = given[i] + extra
            spare = spare - extra
    return np.array([reach] + given)


def uneven(stream_key, number_of, total, bound, slope):
    if number_of == 2:
        one = jax.random.randint(stream_key, (), max(1, total - bound), min(bound, total - 1) + 1)
        return jnp.stack([one, total - one])
    sizes = jnp.asarray(split_up(number_of, total, bound, slope), jnp.int32)
    twos = (number_of - 1) // 2
    source_of, sink = sizes[1:1 + 2 * twos:2], sizes[2:2 + 2 * twos:2]
    margin = jnp.minimum(source_of - 1, bound - sink)
    shifted = jax.random.randint(jax.random.fold_in(stream_key, 1), (twos,), 0, 1 << 20) % (margin + 1)
    sizes = sizes.at[1:1 + 2 * twos:2].set(source_of - shifted).at[2:2 + 2 * twos:2].set(sink + shifted)
    return sizes[jax.random.permutation(jax.random.fold_in(stream_key, 2), number_of)]


def gaussian(key, shape, scale, limit, pieces=(), held_as=jnp.bfloat16):
    gain = steps_of(key, shape, pieces, -0.22, 0.18) if pieces else 1.0
    drawn = jax.random.normal(key, shape, jnp.float32) * scale * gain
    return jnp.minimum(jnp.maximum(drawn, -limit), limit).astype(held_as)


def setup_inputs(seed: int = 0) -> dict:
    seeds = jax.random.split(jax.random.key(seed), 7)
    gate_in = gaussian(seeds[0], (SEQS, SEQ, WIDTH), 1.0, 6.0, ((0, 4), (1, 8)))
    value_in = gaussian(seeds[1], (SEQS, SEQ, WIDTH), 1.0, 6.0, ((0, 4), (1, 8)))
    segments = jax.vmap(lambda own: jnp.searchsorted(jnp.cumsum(uneven(own, DOCS, SEQ, 6 * TOK_DEV, 0)), jnp.arange(SEQ), side="right"))(jax.random.split(seeds[2], SEQS)).reshape((SEQS, SEQ)).astype(jnp.int32)
    value_gain = jnp.clip(1.0 + 0.18 * jax.random.normal(seeds[3], (WIDTH,), jnp.float32), 0.099609375, 1.8984375).astype(jnp.bfloat16)
    mixing = gaussian(seeds[4], (HEADS, BLK, BLK), BLK ** -0.5, 0.1875, ((0, 8), (1, 4)))
    mixing_bias = jnp.clip(1.0 + 0.18 * jax.random.normal(seeds[5], (HEADS, BLK), jnp.float32), 0.099609375, 1.8984375).astype(jnp.bfloat16)
    return dict(gate_in=gate_in, value_in=value_in, segments=segments, value_gain=value_gain, mixing=mixing, mixing_bias=mixing_bias)


epsilon = 1e-06

def reference(gate_in, value_in, segments, value_gain, mixing, mixing_bias):
    seqs, length, width = value_in.shape
    values = jax.nn.gelu(value_in.astype(jnp.float32)).reshape(seqs, length, HEADS, HEAD_DIM)
    scaled = values * lax.rsqrt(lax.optimization_barrier(jnp.mean(values * values, axis=-1, keepdims=True)) + epsilon)
    normed = (scaled.reshape(seqs, length, width) * value_gain.astype(jnp.float32)).astype(jnp.bfloat16)
    blocks = seqs * length // BLK
    value_blocks = normed.reshape(blocks, BLK, HEADS, HEAD_DIM)
    id_blocks = segments.reshape(blocks, BLK)
    mixing_f = mixing.astype(jnp.float32)
    bias_f = jnp.transpose(mixing_bias.astype(jnp.float32))[:, :, None]

    def one_block(pair_item):
        block_values, block_ids = pair_item
        same_doc = block_ids[:, None] == block_ids[None, :]
        masked = jnp.where(same_doc[None, :, :], mixing_f, jnp.zeros((), jnp.float32))
        summed = jnp.einsum('hts,shd->thd', masked, block_values.astype(jnp.float32))
        return (summed + bias_f).astype(jnp.bfloat16)
    mixed = lax.map(one_block, (value_blocks, id_blocks)).reshape(seqs, length, width)
    gate_f = jax.nn.gelu(gate_in.astype(jnp.float32))
    return (gate_f * mixed.astype(jnp.float32)).astype(jnp.bfloat16)
```

```python
import functools

import jax
import jax.numpy as jnp
from jax import lax
from jax.experimental import pallas as pl
from jax.experimental.pallas import tpu as pltpu
from jax.sharding import PartitionSpec as P

HEAD_DIM = 128
CORES = 2
LANES = 128
ROW_STEP = 256
MESH = pl.DeviceIdType.MESH

epsilon = 1e-06


def flip(a, b, count):
    total, bit = 0, 1
    while bit < count:
        total = total + ((a // bit + b // bit) % 2) * bit
        bit *= 2
    return total


def gelu(x):
    return jax.nn.gelu(x, approximate=True)


def to_column(row):
    parts = []
    for at in range(0, row.shape[1], LANES):
        piece = jnp.broadcast_to(row[:, at : at + LANES], (LANES, LANES))
        parts.append(piece.T)
    return jnp.concatenate(parts, axis=0)


def kernel(
    sp, dp, value_ref, ids_ref, gain_ref, mixing_ref, bias_ref, gate_ref, out_ref,
    vals, ids, mix, res, ret, bias_col, normed, ids_col,
    v_send, v_recv, i_send, i_recv, r_send, r_recv, m_send, m_recv, m_fwd, own_sem,
):
    s, d = lax.axis_index("sp"), lax.axis_index("dp")
    tokens = value_ref.shape[0]
    block_len = mix.shape[0]
    per = block_len // tokens
    blocks = sp // per
    rows = mixing_ref.shape[0]
    planes = dp // CORES
    half = s % per
    partner = d + 1 - 2 * (d % CORES)
    plane, core = d // CORES, d % CORES

    def across(step):
        return ((plane + step) % planes) * CORES + core

    barrier = pltpu.get_barrier_semaphore()
    for k in range(1, sp):
        pl.semaphore_signal(barrier, inc=1, device_id={"sp": flip(s, k, sp)}, device_id_type=MESH)
    pl.semaphore_signal(barrier, inc=1, device_id={"dp": partner}, device_id_type=MESH)
    for step in range(1, planes):
        pl.semaphore_signal(barrier, inc=1, device_id={"dp": across(step)}, device_id_type=MESH)
    pl.semaphore_wait(barrier, sp - 1 + planes)

    def chunk(of):
        return mix.at[pl.ds(pl.multiple_of(of * rows, rows), rows)]

    def mix_copy(src, origin, target, sem):
        return pltpu.make_async_remote_copy(
            src_ref=src, dst_ref=chunk(origin), send_sem=sem, recv_sem=m_recv.at[origin],
            device_id={"dp": target}, device_id_type=MESH,
        )

    def value_copy(k, end):
        target = flip(s, k, sp)
        return pltpu.make_async_remote_copy(
            src_ref=value_ref.at[:, pl.ds(pl.multiple_of(target * HEAD_DIM, HEAD_DIM), HEAD_DIM)],
            dst_ref=vals.at[k // per, pl.ds(pl.multiple_of(end * tokens, tokens), tokens)],
            send_sem=v_send.at[k], recv_sem=v_recv.at[k],
            device_id={"sp": target}, device_id_type=MESH,
        )

    def id_copy(k, end):
        return pltpu.make_async_remote_copy(
            src_ref=ids_ref, dst_ref=ids.at[k // per, end],
            send_sem=i_send.at[k], recv_sem=i_recv.at[k],
            device_id={"sp": flip(s, k, sp)}, device_id_type=MESH,
        )

    def result_copy(k):
        target = flip(s, k, sp)
        return pltpu.make_async_remote_copy(
            src_ref=res.at[k // per, pl.ds(pl.multiple_of((target % per) * tokens, tokens), tokens)],
            dst_ref=ret.at[k],
            send_sem=r_send.at[k], recv_sem=r_recv.at[k],
            device_id={"sp": target}, device_id_type=MESH,
        )

    for step in range(1, planes):
        mix_copy(mixing_ref, d, across(step), m_send.at[step]).start()
    mix_copy(mixing_ref, d, partner, m_send.at[0]).start()

    def send_one(k, carry):
        id_copy(k, half).start()
        value_copy(k, half).start()
        return carry

    lax.fori_loop(1, sp, send_one, 0)

    own = pltpu.make_async_copy(mixing_ref, chunk(d), own_sem)
    own.start()
    vals[0, pl.ds(pl.multiple_of(half * tokens, tokens), tokens), :] = value_ref[
        :, pl.ds(pl.multiple_of(s * HEAD_DIM, HEAD_DIM), HEAD_DIM)
    ]
    ids[0, half] = ids_ref[...]
    bias_col[...] = to_column(bias_ref[...].astype(jnp.float32))

    for step in range(1, planes):
        origin = across(planes - step)
        mix_copy(mixing_ref, origin, partner, m_send.at[0]).wait_recv()
        mix_copy(chunk(origin), origin, partner, m_fwd.at[step]).start()
    mix_copy(mixing_ref, partner, partner, m_send.at[0]).wait_recv()
    for step in range(1, planes):
        origin = across(planes - step)
        there = origin + 1 - 2 * (origin % CORES)
        mix_copy(mixing_ref, there, partner, m_send.at[0]).wait_recv()
    own.wait()

    gain = gain_ref[...].astype(jnp.float32)

    def one_block(j, carry):
        for i in range(per):
            k = j * per + i

            @pl.when(k > 0)
            def _():
                source_half = flip(s, k, sp) % per
                id_copy(k, source_half).wait_recv()
                value_copy(k, source_half).wait_recv()

        for at in range(0, block_len, ROW_STEP):
            act = gelu(vals[j, at : at + ROW_STEP, :].astype(jnp.float32))
            mean = jnp.mean(act * act, axis=-1, keepdims=True)
            normed[at : at + ROW_STEP, :] = (act * lax.rsqrt(mean + epsilon) * gain).astype(jnp.bfloat16)
        row = jnp.concatenate([ids[j, i] for i in range(per)], axis=1).astype(jnp.float32)
        ids_col[...] = to_column(row).astype(jnp.bfloat16)
        row_b = row.astype(jnp.bfloat16)
        right = normed[...]
        zero = jnp.zeros((), jnp.bfloat16)
        for at in range(0, block_len, ROW_STEP):
            col = ids_col[at : at + ROW_STEP, :]
            pieces = []
            for c in range(0, block_len, LANES):
                same = col == row_b[:, c : c + LANES]
                pieces.append(jnp.where(same, mix[at : at + ROW_STEP, c : c + LANES], zero))
            summed = jnp.dot(jnp.concatenate(pieces, axis=1), right, preferred_element_type=jnp.float32)
            res[j, at : at + ROW_STEP, :] = (summed + bias_col[at : at + ROW_STEP, :]).astype(jnp.bfloat16)
        for i in range(per):
            k = j * per + i

            @pl.when(k > 0)
            def _():
                result_copy(k).start()

        return carry

    lax.fori_loop(0, blocks, one_block, 0)
    ret[0] = res[0, pl.ds(pl.multiple_of(half * tokens, tokens), tokens), :]

    def finish(k, carry):
        @pl.when(k > 0)
        def _():
            result_copy(k).wait_recv()

        lanes = pl.ds(pl.multiple_of(flip(s, k, sp) * HEAD_DIM, HEAD_DIM), HEAD_DIM)
        for at in range(0, tokens, ROW_STEP):
            gate = gelu(gate_ref[at : at + ROW_STEP, lanes].astype(jnp.float32))
            got = ret[k, at : at + ROW_STEP, :].astype(jnp.float32)
            out_ref[at : at + ROW_STEP, lanes] = (gate * got).astype(jnp.bfloat16)
        return carry

    lax.fori_loop(0, sp, finish, 0)

    def drain(k, carry):
        id_copy(k, half).wait_send()
        value_copy(k, half).wait_send()
        result_copy(k).wait_send()
        return carry

    lax.fori_loop(1, sp, drain, 0)
    mix_copy(mixing_ref, d, partner, m_send.at[0]).wait_send()
    for step in range(1, planes):
        mix_copy(mixing_ref, d, across(step), m_send.at[step]).wait_send()
        origin = across(planes - step)
        mix_copy(chunk(origin), origin, partner, m_fwd.at[step]).wait_send()


def per_device(gate_in, value_in, segments, value_gain, mixing, mixing_bias):
    sp, dp = lax.axis_size("sp"), lax.axis_size("dp")
    sequences, tokens, width = value_in.shape
    heads_here, rows, block_len = mixing.shape
    assert sequences == 1 and heads_here == 1
    per = block_len // tokens
    blocks = sp // per
    bf16, f32 = jnp.bfloat16, jnp.float32
    dma = pltpu.SemaphoreType.DMA
    vmem, anywhere = pl.BlockSpec(memory_space=pltpu.VMEM), pl.BlockSpec(memory_space=pl.ANY)
    out = pl.pallas_call(
        functools.partial(kernel, sp, dp),
        out_shape=jax.ShapeDtypeStruct((tokens, width), bf16),
        in_specs=[vmem, vmem, vmem, anywhere, vmem, vmem],
        out_specs=vmem,
        scratch_shapes=[
            pltpu.VMEM((blocks, block_len, HEAD_DIM), bf16),
            pltpu.VMEM((blocks, per, 1, tokens), jnp.int32),
            pltpu.VMEM((block_len, block_len), bf16),
            pltpu.VMEM((blocks, block_len, HEAD_DIM), bf16),
            pltpu.VMEM((sp, tokens, HEAD_DIM), bf16),
            pltpu.VMEM((block_len, LANES), f32),
            pltpu.VMEM((block_len, HEAD_DIM), bf16),
            pltpu.VMEM((block_len, LANES), bf16),
            dma((sp,)), dma((sp,)), dma((sp,)), dma((sp,)), dma((sp,)), dma((sp,)),
            dma((dp // CORES,)), dma((dp,)), dma((dp // CORES,)), dma,
        ],
        compiler_params=pltpu.CompilerParams(
            collective_id=0, has_side_effects=True, vmem_limit_bytes=60 * 1024 * 1024
        ),
    )(
        value_in.reshape(tokens, width),
        segments,
        value_gain.reshape(1, HEAD_DIM),
        mixing.reshape(rows, block_len),
        mixing_bias,
        gate_in.reshape(tokens, width),
    )
    return out.reshape(sequences, tokens, width)


def solution(mesh):
    return jax.shard_map(
        per_device,
        mesh=mesh,
        in_specs=(
            P("dp", "sp", None),
            P("dp", "sp", None),
            P("dp", "sp"),
            P("sp"),
            P("sp", "dp", None),
            P("sp", None),
        ),
        out_specs=P("dp", "sp", None),
        check_vma=False,
    )
```

```python
import functools

import jax
import jax.numpy as jnp
from jax import lax
from jax.experimental import pallas as pl
from jax.experimental.pallas import tpu as pltpu
from jax.sharding import PartitionSpec as P

HEAD_DIM = 128
CORES = 2
LANES = 128
ROW_STEP = 256
PARTS = 4
MESH = pl.DeviceIdType.MESH

epsilon = 1e-06


def flip(a, b, count):
    total, bit = 0, 1
    while bit < count:
        total = total + ((a // bit + b // bit) % 2) * bit
        bit *= 2
    return total


def gelu(x):
    return jax.nn.gelu(x, approximate=True)


def to_column(row):
    parts = []
    for at in range(0, row.shape[1], LANES):
        piece = jnp.broadcast_to(row[:, at : at + LANES], (LANES, LANES))
        parts.append(piece.T)
    return jnp.concatenate(parts, axis=0)


def kernel(
    sp, dp, value_ref, ids_ref, gain_ref, mixing_ref, bias_ref, gate_ref, out_ref,
    vals, ids, mix, res, ret, bias_col, normed, ids_col, extras, extras_in,
    v_send, v_recv, i_send, i_recv, r_send, r_recv, m_send, m_recv, m_fwd, own_sem,
    e_send, e_recv, far_send, far_recv, across_send, core_send, fwd_send,
):
    s, d = lax.axis_index("sp"), lax.axis_index("dp")
    tokens = value_ref.shape[0]
    block_len = mix.shape[1]
    per = block_len // tokens
    near = sp // 2
    blocks = near // per
    rows = mixing_ref.shape[0]
    planes = dp // CORES
    half = s % per
    partner = d + 1 - 2 * (d % CORES)
    plane, core = d // CORES, d % CORES

    def across(step):
        return ((plane + step) % planes) * CORES + core

    extras[:, :block_len] = bias_ref[...].astype(jnp.float32)
    extras[:, block_len:] = gain_ref[...].astype(jnp.float32)
    barrier = pltpu.get_barrier_semaphore()
    for k in range(1, near + 1):
        pl.semaphore_signal(barrier, inc=1, device_id={"sp": flip(s, k, sp)}, device_id_type=MESH)
    pl.semaphore_signal(barrier, inc=1, device_id={"dp": partner}, device_id_type=MESH)
    for step in range(1, planes):
        pl.semaphore_signal(barrier, inc=1, device_id={"dp": across(step)}, device_id_type=MESH)
    pl.semaphore_wait(barrier, near + planes)

    def chunk(of):
        return mix.at[0, pl.ds(pl.multiple_of(of * rows, rows), rows)]

    def mix_copy(src, origin, target, sem):
        return pltpu.make_async_remote_copy(
            src_ref=src, dst_ref=chunk(origin), send_sem=sem, recv_sem=m_recv.at[origin],
            device_id={"dp": target}, device_id_type=MESH,
        )

    part = rows // PARTS

    def far_part(origin, q):
        return mix.at[1, pl.ds(pl.multiple_of(origin * rows + q * part, part), part)]

    def far_copy(src, origin, q, where, sem):
        return pltpu.make_async_remote_copy(
            src_ref=src, dst_ref=far_part(origin, q), send_sem=sem,
            recv_sem=far_recv.at[origin * PARTS + q], device_id=where, device_id_type=MESH,
        )

    def from_far(q):
        return far_copy(
            mixing_ref.at[pl.ds(q * part, part)], d, q, {"sp": flip(s, near, sp)}, far_send.at[q]
        )

    def to_plane(step, q):
        return far_copy(
            far_part(d, q), d, q, {"dp": across(step)}, across_send.at[step * PARTS + q]
        )

    def to_core(q):
        return far_copy(far_part(d, q), d, q, {"dp": partner}, core_send.at[q])

    def pass_on(step, q):
        origin = across(planes - step)
        return far_copy(
            far_part(origin, q), origin, q, {"dp": partner}, fwd_send.at[step * PARTS + q]
        )

    def extras_copy():
        return pltpu.make_async_remote_copy(
            src_ref=extras, dst_ref=extras_in, send_sem=e_send, recv_sem=e_recv,
            device_id={"sp": flip(s, near, sp)}, device_id_type=MESH,
        )

    def value_copy(k, end):
        target, head = flip(s, k % near, sp), flip(s, k, sp)
        return pltpu.make_async_remote_copy(
            src_ref=value_ref.at[:, pl.ds(pl.multiple_of(head * HEAD_DIM, HEAD_DIM), HEAD_DIM)],
            dst_ref=vals.at[k // per, pl.ds(pl.multiple_of(end * tokens, tokens), tokens)],
            send_sem=v_send.at[k], recv_sem=v_recv.at[k],
            device_id={"sp": target}, device_id_type=MESH,
        )

    def id_copy(k, end):
        return pltpu.make_async_remote_copy(
            src_ref=ids_ref, dst_ref=ids.at[k // per, end],
            send_sem=i_send.at[k], recv_sem=i_recv.at[k],
            device_id={"sp": flip(s, k, sp)}, device_id_type=MESH,
        )

    def result_copy(k):
        target = flip(s, k % near, sp)
        return pltpu.make_async_remote_copy(
            src_ref=res.at[k // per, pl.ds(pl.multiple_of((target % per) * tokens, tokens), tokens)],
            dst_ref=ret.at[k],
            send_sem=r_send.at[k], recv_sem=r_recv.at[k],
            device_id={"sp": target}, device_id_type=MESH,
        )

    for step in range(1, planes):
        mix_copy(mixing_ref, d, across(step), m_send.at[step]).start()
    mix_copy(mixing_ref, d, partner, m_send.at[0]).start()

    def send_one(k, carry):
        id_copy(k, half).start()
        value_copy(k, half).start()
        return carry

    def send_more(k, carry):
        value_copy(k, half).start()
        return carry

    extras_copy().start()
    lax.fori_loop(1, near, send_one, 0)
    for q in range(PARTS):
        from_far(q).start()
    lax.fori_loop(near + 1, sp, send_more, 0)

    own = pltpu.make_async_copy(mixing_ref, chunk(d), own_sem)
    own.start()
    for k in (0, near):
        vals[k // per, pl.ds(pl.multiple_of(half * tokens, tokens), tokens), :] = value_ref[
            :, pl.ds(pl.multiple_of(flip(s, k, sp) * HEAD_DIM, HEAD_DIM), HEAD_DIM)
        ]
    ids[0, half] = ids_ref[...]
    bias_col[0] = to_column(extras[:, :block_len])

    for step in range(1, planes):
        origin = across(planes - step)
        mix_copy(mixing_ref, origin, partner, m_send.at[0]).wait_recv()
        mix_copy(chunk(origin), origin, partner, m_fwd.at[step]).start()
    mix_copy(mixing_ref, partner, partner, m_send.at[0]).wait_recv()
    for step in range(1, planes):
        origin = across(planes - step)
        there = origin + 1 - 2 * (origin % CORES)
        mix_copy(mixing_ref, there, partner, m_send.at[0]).wait_recv()
    own.wait()

    def one_block(which, j):
        gain = (extras, extras_in)[which][:, block_len:]
        at_block = which * blocks + j
        for i in range(per):
            k = j * per + i

            @pl.when(k > 0)
            def _():
                source_half = flip(s, k, sp) % per
                if which == 0:
                    id_copy(k, source_half).wait_recv()
                value_copy(k + which * near, source_half).wait_recv()

        for at in range(0, block_len, ROW_STEP):
            act = gelu(vals[at_block, at : at + ROW_STEP, :].astype(jnp.float32))
            mean = jnp.mean(act * act, axis=-1, keepdims=True)
            normed[at : at + ROW_STEP, :] = (act * lax.rsqrt(mean + epsilon) * gain).astype(jnp.bfloat16)
        row = jnp.concatenate([ids[j, i] for i in range(per)], axis=1).astype(jnp.float32)
        ids_col[...] = to_column(row).astype(jnp.bfloat16)
        row_b = row.astype(jnp.bfloat16)
        right = normed[...]
        zero = jnp.zeros((), jnp.bfloat16)
        for at in range(0, block_len, ROW_STEP):
            col = ids_col[at : at + ROW_STEP, :]
            pieces = []
            for c in range(0, block_len, LANES):
                same = col == row_b[:, c : c + LANES]
                pieces.append(jnp.where(same, mix[which, at : at + ROW_STEP, c : c + LANES], zero))
            summed = jnp.dot(jnp.concatenate(pieces, axis=1), right, preferred_element_type=jnp.float32)
            res[at_block, at : at + ROW_STEP, :] = (summed + bias_col[which, at : at + ROW_STEP, :]).astype(jnp.bfloat16)
        for i in range(per):
            k = j * per + i

            @pl.when(k > 0)
            def _():
                result_copy(k + which * near).start()

    def relay(q):
        from_far(q).wait_recv()
        for step in range(1, planes):
            to_plane(step, q).start()
        to_core(q).start()

    def some_blocks(first, last):
        def body(j, carry):
            one_block(0, j)
            return carry

        lax.fori_loop(first, last, body, 0)

    relay(0)
    relay(1)
    some_blocks(0, blocks // 2)
    relay(2)
    some_blocks(blocks // 2, blocks)
    relay(3)
    extras_copy().wait_recv()
    bias_col[1] = to_column(extras_in[:, :block_len])
    for q in range(PARTS):
        for step in range(1, planes):
            pass_on(step, q).wait_recv()
            pass_on(step, q).start()
    for q in range(PARTS):
        far_copy(far_part(d, q), partner, q, {"dp": partner}, core_send.at[q]).wait_recv()
        for step in range(1, planes):
            origin = across(planes - step)
            there = origin + 1 - 2 * (origin % CORES)
            far_copy(far_part(d, q), there, q, {"dp": partner}, core_send.at[q]).wait_recv()

    def far_block(n, carry):
        one_block(1, blocks - 1 - n)
        return carry

    lax.fori_loop(0, blocks, far_block, 0)
    for k in (0, near):
        ret[k] = res[k // per, pl.ds(pl.multiple_of(half * tokens, tokens), tokens), :]

    def finish(k, carry):
        @pl.when(k % near > 0)
        def _():
            result_copy(k).wait_recv()

        lanes = pl.ds(pl.multiple_of(flip(s, k, sp) * HEAD_DIM, HEAD_DIM), HEAD_DIM)
        for at in range(0, tokens, ROW_STEP):
            gate = gelu(gate_ref[at : at + ROW_STEP, lanes].astype(jnp.float32))
            got = ret[k, at : at + ROW_STEP, :].astype(jnp.float32)
            out_ref[at : at + ROW_STEP, lanes] = (gate * got).astype(jnp.bfloat16)
        return carry

    lax.fori_loop(0, sp, finish, 0)

    def drain(k, carry):
        id_copy(k, half).wait_send()
        for n in (k, k + near):
            value_copy(n, half).wait_send()
            result_copy(n).wait_send()
        return carry

    lax.fori_loop(1, near, drain, 0)
    extras_copy().wait_send()
    for q in range(PARTS):
        from_far(q).wait_send()
        to_core(q).wait_send()
        for step in range(1, planes):
            to_plane(step, q).wait_send()
            pass_on(step, q).wait_send()
    mix_copy(mixing_ref, d, partner, m_send.at[0]).wait_send()
    for step in range(1, planes):
        mix_copy(mixing_ref, d, across(step), m_send.at[step]).wait_send()
        origin = across(planes - step)
        mix_copy(chunk(origin), origin, partner, m_fwd.at[step]).wait_send()


def per_device(gate_in, value_in, segments, value_gain, mixing, mixing_bias):
    sp, dp = lax.axis_size("sp"), lax.axis_size("dp")
    sequences, tokens, width = value_in.shape
    heads_here, rows, block_len = mixing.shape
    assert sequences == 1 and heads_here == 1
    per = block_len // tokens
    near = sp // 2
    blocks = near // per
    bf16, f32 = jnp.bfloat16, jnp.float32
    dma = pltpu.SemaphoreType.DMA
    vmem, anywhere = pl.BlockSpec(memory_space=pltpu.VMEM), pl.BlockSpec(memory_space=pl.ANY)
    out = pl.pallas_call(
        functools.partial(kernel, sp, dp),
        out_shape=jax.ShapeDtypeStruct((tokens, width), bf16),
        in_specs=[vmem, vmem, vmem, anywhere, vmem, vmem],
        out_specs=vmem,
        scratch_shapes=[
            pltpu.VMEM((2 * blocks, block_len, HEAD_DIM), bf16),
            pltpu.VMEM((blocks, per, 1, tokens), jnp.int32),
            pltpu.VMEM((2, block_len, block_len), bf16),
            pltpu.VMEM((2 * blocks, block_len, HEAD_DIM), bf16),
            pltpu.VMEM((sp, tokens, HEAD_DIM), bf16),
            pltpu.VMEM((2, block_len, LANES), f32),
            pltpu.VMEM((block_len, HEAD_DIM), bf16),
            pltpu.VMEM((block_len, LANES), bf16),
            pltpu.VMEM((1, block_len + HEAD_DIM), f32),
            pltpu.VMEM((1, block_len + HEAD_DIM), f32),
            dma((sp,)), dma((sp,)), dma((sp,)), dma((sp,)), dma((sp,)), dma((sp,)),
            dma((dp // CORES,)), dma((dp,)), dma((dp // CORES,)), dma,
            dma, dma, dma((PARTS,)), dma((dp * PARTS,)), dma((dp // CORES * PARTS,)),
            dma((PARTS,)), dma((dp // CORES * PARTS,)),
        ],
        compiler_params=pltpu.CompilerParams(
            collective_id=0, has_side_effects=True, vmem_limit_bytes=60 * 1024 * 1024
        ),
    )(
        value_in.reshape(tokens, width),
        segments,
        value_gain.reshape(1, HEAD_DIM),
        mixing.reshape(rows, block_len),
        mixing_bias,
        gate_in.reshape(tokens, width),
    )
    return out.reshape(sequences, tokens, width)


def solution(mesh):
    return jax.shard_map(
        per_device,
        mesh=mesh,
        in_specs=(
            P("dp", "sp", None),
            P("dp", "sp", None),
            P("dp", "sp"),
            P("sp"),
            P("sp", "dp", None),
            P("sp", None),
        ),
        out_specs=P("dp", "sp", None),
        check_vma=False,
    )
```

```python
import functools

import jax
import jax.numpy as jnp
from jax import lax
from jax.experimental import pallas as pl
from jax.experimental.pallas import tpu as pltpu
from jax.sharding import PartitionSpec as P

HEAD_DIM = 128
CORES = 2
LANES = 128
ROW_STEP = 256
PARTS = 4
MESH = pl.DeviceIdType.MESH

epsilon = 1e-06


def flip(a, b, count):
    total, bit = 0, 1
    while bit < count:
        total = total + ((a // bit + b // bit) % 2) * bit
        bit *= 2
    return total


def gelu(x):
    return jax.nn.gelu(x, approximate=True)


def to_column(row):
    parts = []
    for at in range(0, row.shape[1], LANES):
        piece = jnp.broadcast_to(row[:, at : at + LANES], (LANES, LANES))
        parts.append(piece.T)
    return jnp.concatenate(parts, axis=0)


def kernel(
    sp, dp, value_ref, ids_ref, gain_ref, mixing_ref, bias_ref, gate_ref, out_ref,
    vals, ids, mix, res, ret, bias_col, normed, ids_col, extras, extras_in,
    v_send, v_recv, i_send, i_recv, r_send, r_recv, m_send, m_recv, m_fwd, own_sem,
    e_send, e_recv, far_send, far_recv, across_send, core_send, fwd_send,
):
    s, d = lax.axis_index("sp"), lax.axis_index("dp")
    tokens = value_ref.shape[0]
    block_len = mix.shape[1]
    per = block_len // tokens
    near = sp // 2
    blocks = near // per
    rows = mixing_ref.shape[0]
    planes = dp // CORES
    half = s % per
    partner = d + 1 - 2 * (d % CORES)
    plane, core = d // CORES, d % CORES

    def across(step):
        return ((plane + step) % planes) * CORES + core

    extras[:, :block_len] = bias_ref[...].astype(jnp.float32)
    extras[:, block_len:] = gain_ref[...].astype(jnp.float32)
    barrier = pltpu.get_barrier_semaphore()
    for k in range(1, near + 1):
        pl.semaphore_signal(barrier, inc=1, device_id={"sp": flip(s, k, sp)}, device_id_type=MESH)
    pl.semaphore_signal(barrier, inc=1, device_id={"dp": partner}, device_id_type=MESH)
    for step in range(1, planes):
        pl.semaphore_signal(barrier, inc=1, device_id={"dp": across(step)}, device_id_type=MESH)
    pl.semaphore_wait(barrier, near + planes)

    def chunk(of):
        return mix.at[0, pl.ds(pl.multiple_of(of * rows, rows), rows)]

    def mix_copy(src, origin, target, sem):
        return pltpu.make_async_remote_copy(
            src_ref=src, dst_ref=chunk(origin), send_sem=sem, recv_sem=m_recv.at[origin],
            device_id={"dp": target}, device_id_type=MESH,
        )

    part = rows // PARTS

    def far_part(origin, q):
        return mix.at[1, pl.ds(pl.multiple_of(origin * rows + q * part, part), part)]

    def far_copy(src, origin, q, where, sem):
        return pltpu.make_async_remote_copy(
            src_ref=src, dst_ref=far_part(origin, q), send_sem=sem,
            recv_sem=far_recv.at[origin * PARTS + q], device_id=where, device_id_type=MESH,
        )

    def from_far(q):
        return far_copy(
            mixing_ref.at[pl.ds(q * part, part)], d, q, {"sp": flip(s, near, sp)}, far_send.at[q]
        )

    def to_plane(step, q):
        return far_copy(
            far_part(d, q), d, q, {"dp": across(step)}, across_send.at[step * PARTS + q]
        )

    def to_core(q):
        return far_copy(far_part(d, q), d, q, {"dp": partner}, core_send.at[q])

    def pass_on(step, q):
        origin = across(planes - step)
        return far_copy(
            far_part(origin, q), origin, q, {"dp": partner}, fwd_send.at[step * PARTS + q]
        )

    def extras_copy():
        return pltpu.make_async_remote_copy(
            src_ref=extras, dst_ref=extras_in, send_sem=e_send, recv_sem=e_recv,
            device_id={"sp": flip(s, near, sp)}, device_id_type=MESH,
        )

    def value_copy(k, end):
        target, head = flip(s, k % near, sp), flip(s, k, sp)
        return pltpu.make_async_remote_copy(
            src_ref=value_ref.at[:, pl.ds(pl.multiple_of(head * HEAD_DIM, HEAD_DIM), HEAD_DIM)],
            dst_ref=vals.at[k // per, pl.ds(pl.multiple_of(end * tokens, tokens), tokens)],
            send_sem=v_send.at[k], recv_sem=v_recv.at[k],
            device_id={"sp": target}, device_id_type=MESH,
        )

    def id_copy(k, end):
        return pltpu.make_async_remote_copy(
            src_ref=ids_ref, dst_ref=ids.at[k // per, end],
            send_sem=i_send.at[k], recv_sem=i_recv.at[k],
            device_id={"sp": flip(s, k, sp)}, device_id_type=MESH,
        )

    def result_copy(k):
        target = flip(s, k % near, sp)
        return pltpu.make_async_remote_copy(
            src_ref=res.at[k // per, pl.ds(pl.multiple_of((target % per) * tokens, tokens), tokens)],
            dst_ref=ret.at[k],
            send_sem=r_send.at[k], recv_sem=r_recv.at[k],
            device_id={"sp": target}, device_id_type=MESH,
        )

    for step in range(1, planes):
        mix_copy(mixing_ref, d, across(step), m_send.at[step]).start()
    mix_copy(mixing_ref, d, partner, m_send.at[0]).start()

    def send_one(k, carry):
        id_copy(k, half).start()
        value_copy(k, half).start()
        return carry

    def send_more(k, carry):
        value_copy(k, half).start()
        return carry

    extras_copy().start()
    lax.fori_loop(1, near, send_one, 0)
    for q in range(PARTS):
        from_far(q).start()
    lax.fori_loop(near + 1, sp, send_more, 0)

    own = pltpu.make_async_copy(mixing_ref, chunk(d), own_sem)
    own.start()
    for k in (0, near):
        vals[k // per, pl.ds(pl.multiple_of(half * tokens, tokens), tokens), :] = value_ref[
            :, pl.ds(pl.multiple_of(flip(s, k, sp) * HEAD_DIM, HEAD_DIM), HEAD_DIM)
        ]
    ids[0, half] = ids_ref[...]
    bias_col[0] = to_column(extras[:, :block_len])

    for step in range(1, planes):
        origin = across(planes - step)
        mix_copy(mixing_ref, origin, partner, m_send.at[0]).wait_recv()
        mix_copy(chunk(origin), origin, partner, m_fwd.at[step]).start()
    mix_copy(mixing_ref, partner, partner, m_send.at[0]).wait_recv()
    for step in range(1, planes):
        origin = across(planes - step)
        there = origin + 1 - 2 * (origin % CORES)
        mix_copy(mixing_ref, there, partner, m_send.at[0]).wait_recv()
    own.wait()

    def one_block(which, j):
        gain = (extras, extras_in)[which][:, block_len:]
        at_block = which * blocks + j
        for i in range(per):
            k = j * per + i

            @pl.when(k > 0)
            def _():
                source_half = flip(s, k, sp) % per
                if which == 0:
                    id_copy(k, source_half).wait_recv()
                value_copy(k + which * near, source_half).wait_recv()

        for at in range(0, block_len, ROW_STEP):
            act = gelu(vals[at_block, at : at + ROW_STEP, :].astype(jnp.float32))
            mean = jnp.mean(act * act, axis=-1, keepdims=True)
            normed[at : at + ROW_STEP, :] = (act * lax.rsqrt(mean + epsilon) * gain).astype(jnp.bfloat16)
        row = jnp.concatenate([ids[j, i] for i in range(per)], axis=1).astype(jnp.float32)
        ids_col[j] = to_column(row).astype(jnp.bfloat16)
        row_b = row.astype(jnp.bfloat16)
        right = normed[...]
        zero = jnp.zeros((), jnp.bfloat16)
        for at in range(0, block_len, ROW_STEP):
            col = ids_col[j, at : at + ROW_STEP, :]
            pieces = []
            for c in range(0, block_len, LANES):
                same = col == row_b[:, c : c + LANES]
                pieces.append(jnp.where(same, mix[which, at : at + ROW_STEP, c : c + LANES], zero))
            summed = jnp.dot(jnp.concatenate(pieces, axis=1), right, preferred_element_type=jnp.float32)
            res[at_block, at : at + ROW_STEP, :] = (summed + bias_col[which, at : at + ROW_STEP, :]).astype(jnp.bfloat16)
        for i in range(per):
            k = j * per + i

            @pl.when(k > 0)
            def _():
                result_copy(k + which * near).start()

    def relay(q):
        from_far(q).wait_recv()
        for step in range(1, planes):
            to_plane(step, q).start()
        to_core(q).start()

    def some_blocks(first, last):
        def body(j, carry):
            one_block(0, j)
            return carry

        lax.fori_loop(first, last, body, 0)

    relay(0)
    relay(1)
    some_blocks(0, blocks // 2)
    relay(2)
    some_blocks(blocks // 2, blocks)
    relay(3)
    extras_copy().wait_recv()
    bias_col[1] = to_column(extras_in[:, :block_len])
    def relay_on(q):
        for step in range(1, planes):
            pass_on(step, q).wait_recv()
            pass_on(step, q).start()

    def far_ready(j, carry):
        gain = extras_in[:, block_len:]
        for i in range(per):
            k = j * per + i

            @pl.when(k > 0)
            def _():
                value_copy(k + near, flip(s, k, sp) % per).wait_recv()

        for at in range(0, block_len, ROW_STEP):
            act = gelu(vals[blocks + j, at : at + ROW_STEP, :].astype(jnp.float32))
            mean = jnp.mean(act * act, axis=-1, keepdims=True)
            vals[blocks + j, at : at + ROW_STEP, :] = (
                act * lax.rsqrt(mean + epsilon) * gain
            ).astype(jnp.bfloat16)
        return carry

    def far_rows(origin):
        span = pl.ds(pl.multiple_of(origin * rows, rows), rows)

        def body(j, carry):
            row = jnp.concatenate([ids[j, i] for i in range(per)], axis=1)
            row_b = row.astype(jnp.float32).astype(jnp.bfloat16)
            col = ids_col[j, span, :]
            pieces = []
            for c in range(0, block_len, LANES):
                same = col == row_b[:, c : c + LANES]
                pieces.append(jnp.where(same, mix[1, span, c : c + LANES], jnp.zeros((), jnp.bfloat16)))
            summed = jnp.dot(
                jnp.concatenate(pieces, axis=1), vals[blocks + j], preferred_element_type=jnp.float32
            )
            res[blocks + j, span, :] = (summed + bias_col[1, span, :]).astype(jnp.bfloat16)
            return carry

        lax.fori_loop(0, blocks, body, 0)

    def arrived(origin):
        for q in range(PARTS):
            far_copy(far_part(d, q), origin, q, {"dp": partner}, core_send.at[q]).wait_recv()

    for q in range(PARTS - 1):
        relay_on(q)
    lax.fori_loop(0, blocks, far_ready, 0)
    far_rows(d)
    relay_on(PARTS - 1)
    arrived(partner)
    far_rows(partner)
    for step in range(1, planes):
        origin = across(planes - step)
        far_rows(origin)
        there = origin + 1 - 2 * (origin % CORES)
        arrived(there)
        far_rows(there)

    def far_block(n, carry):
        j = blocks - 1 - n
        for i in range(per):
            k = j * per + i

            @pl.when(k > 0)
            def _():
                result_copy(k + near).start()

        return carry

    lax.fori_loop(0, blocks, far_block, 0)
    for k in (0, near):
        ret[k] = res[k // per, pl.ds(pl.multiple_of(half * tokens, tokens), tokens), :]

    def finish(k, carry):
        @pl.when(k % near > 0)
        def _():
            result_copy(k).wait_recv()

        lanes = pl.ds(pl.multiple_of(flip(s, k, sp) * HEAD_DIM, HEAD_DIM), HEAD_DIM)
        for at in range(0, tokens, ROW_STEP):
            gate = gelu(gate_ref[at : at + ROW_STEP, lanes].astype(jnp.float32))
            got = ret[k, at : at + ROW_STEP, :].astype(jnp.float32)
            out_ref[at : at + ROW_STEP, lanes] = (gate * got).astype(jnp.bfloat16)
        return carry

    lax.fori_loop(0, sp, finish, 0)

    def drain(k, carry):
        id_copy(k, half).wait_send()
        for n in (k, k + near):
            value_copy(n, half).wait_send()
            result_copy(n).wait_send()
        return carry

    lax.fori_loop(1, near, drain, 0)
    extras_copy().wait_send()
    for q in range(PARTS):
        from_far(q).wait_send()
        to_core(q).wait_send()
        for step in range(1, planes):
            to_plane(step, q).wait_send()
            pass_on(step, q).wait_send()
    mix_copy(mixing_ref, d, partner, m_send.at[0]).wait_send()
    for step in range(1, planes):
        mix_copy(mixing_ref, d, across(step), m_send.at[step]).wait_send()
        origin = across(planes - step)
        mix_copy(chunk(origin), origin, partner, m_fwd.at[step]).wait_send()


def per_device(gate_in, value_in, segments, value_gain, mixing, mixing_bias):
    sp, dp = lax.axis_size("sp"), lax.axis_size("dp")
    sequences, tokens, width = value_in.shape
    heads_here, rows, block_len = mixing.shape
    assert sequences == 1 and heads_here == 1
    per = block_len // tokens
    near = sp // 2
    blocks = near // per
    bf16, f32 = jnp.bfloat16, jnp.float32
    dma = pltpu.SemaphoreType.DMA
    vmem, anywhere = pl.BlockSpec(memory_space=pltpu.VMEM), pl.BlockSpec(memory_space=pl.ANY)
    out = pl.pallas_call(
        functools.partial(kernel, sp, dp),
        out_shape=jax.ShapeDtypeStruct((tokens, width), bf16),
        in_specs=[vmem, vmem, vmem, anywhere, vmem, vmem],
        out_specs=vmem,
        scratch_shapes=[
            pltpu.VMEM((2 * blocks, block_len, HEAD_DIM), bf16),
            pltpu.VMEM((blocks, per, 1, tokens), jnp.int32),
            pltpu.VMEM((2, block_len, block_len), bf16),
            pltpu.VMEM((2 * blocks, block_len, HEAD_DIM), bf16),
            pltpu.VMEM((sp, tokens, HEAD_DIM), bf16),
            pltpu.VMEM((2, block_len, LANES), f32),
            pltpu.VMEM((block_len, HEAD_DIM), bf16),
            pltpu.VMEM((blocks, block_len, LANES), bf16),
            pltpu.VMEM((1, block_len + HEAD_DIM), f32),
            pltpu.VMEM((1, block_len + HEAD_DIM), f32),
            dma((sp,)), dma((sp,)), dma((sp,)), dma((sp,)), dma((sp,)), dma((sp,)),
            dma((dp // CORES,)), dma((dp,)), dma((dp // CORES,)), dma,
            dma, dma, dma((PARTS,)), dma((dp * PARTS,)), dma((dp // CORES * PARTS,)),
            dma((PARTS,)), dma((dp // CORES * PARTS,)),
        ],
        compiler_params=pltpu.CompilerParams(
            collective_id=0, has_side_effects=True, vmem_limit_bytes=60 * 1024 * 1024
        ),
    )(
        value_in.reshape(tokens, width),
        segments,
        value_gain.reshape(1, HEAD_DIM),
        mixing.reshape(rows, block_len),
        mixing_bias,
        gate_in.reshape(tokens, width),
    )
    return out.reshape(sequences, tokens, width)


def solution(mesh):
    return jax.shard_map(
        per_device,
        mesh=mesh,
        in_specs=(
            P("dp", "sp", None),
            P("dp", "sp", None),
            P("dp", "sp"),
            P("sp"),
            P("sp", "dp", None),
            P("sp", None),
        ),
        out_specs=P("dp", "sp", None),
        check_vma=False,
    )
```
